32 devices in a mesh: fs: 8 (over z, y), tp: 4 (over x, core).
Axes of the slice: x: 2, y: 2, z: 4, core: 2. Of those that a mesh axis runs over, the one named last changes fastest.
Arguments:
- x_next: bfloat16 [1536, 2048], P(('fs', 'tp')), may hold values from -6 to 6
- x_prev: bfloat16 [1536, 2048], P(('fs', 'tp')), may hold values from -6 to 6
- grad_out: bfloat16 [1536, 2048], P(('fs', 'tp')), may hold values from -6 to 6
- gate_w: bfloat16 [2048, 2816], P('fs', 'tp'), may hold values from -0.125 to 0.125
- up_w: bfloat16 [2048, 2816], P('fs', 'tp'), may hold values from -0.125 to 0.125
- down_w: bfloat16 [2816, 2048], P('tp', 'fs'), may hold values from -0.109375 to 0.109375
- acc_gate: float32 [2048, 2816], P('fs', 'tp'), may hold values from -2.5 to 2.5
- acc_up: float32 [2048, 2816], P('fs', 'tp'), may hold values from -2.5 to 2.5
- acc_down: float32 [2816, 2048], P('tp', 'fs'), may hold values from -2.5 to 2.5
Outputs:
- out_next: bfloat16 [1536, 2048], P(('fs', 'tp'))
- saved_hidden: bfloat16 [1536, 2816], P('fs', 'tp')
- grad_input: bfloat16 [1536, 2048], P(('fs', 'tp'))
- new_gate: float32 [2048, 2816], P('fs', 'tp')
- new_up: float32 [2048, 2816], P('fs', 'tp')
- new_down: float32 [2816, 2048], P('tp', 'fs')
The draws below stay inside these ranges and needn't reach their ends.
All inputs are finite; a program needn't handle non-finite values.
Results may differ from the reference program's by a relative error of at most 0.014.
Values may be sent and summed in bfloat16 or wider, within the bound.
A program may use at most 64 MiB of HBM per device.

```python
import math
import jax
import jax.numpy as jnp
from jax import lax

D = 2048
FF = 2816
TOKENS = 1536
N_TP = 4


def spiked(drawn, rng, source, target, shards_of, factor):
    owner, partner = [(jnp.arange(drawn.shape[dim]) // (drawn.shape[dim] // shards_of)).reshape([-1 if axis == dim else 1 for axis in range(drawn.ndim)]) for dim in (source, target)]
    chosen = jax.random.permutation(rng, shards_of)[partner]
    strong = (owner == chosen) | (owner == (partner + shards_of // 2) % shards_of)
    return jnp.where(strong, factor * drawn, drawn)


def block_scale(key, extent, pieces, smallest, top_value):
    def one(axis_at, shards_of):
        draws = jax.random.uniform(jax.random.fold_in(jax.random.fold_in(key, 6), axis_at), (shards_of,), jnp.float32, smallest / len(pieces), top_value / len(pieces))
        return jnp.repeat(jnp.exp(draws), extent[axis_at] // shards_of).reshape((-1,) + (1,) * (len(extent) - axis_at - 1))

    loudness = one(*pieces[0])
    for cut in pieces[1:]:
        loudness = loudness * one(*cut)
    return loudness


def centred(own_key, dims, spread, bound, pieces=(), dtype=jnp.bfloat16):
    level = block_scale(own_key, dims, pieces, -0.22, 0.18) if pieces else 1.0
    entries = jax.random.normal(own_key, dims, jnp.float32) * spread * level
    return jnp.minimum(jnp.maximum(entries, -bound), bound).astype(dtype)


def heavy_noise(rng, shape, spread, limit, pieces, heavy, kind=jnp.bfloat16):
    entries = spread * jax.random.normal(rng, shape, jnp.float32)
    if pieces:
        entries = entries * block_scale(rng, shape, pieces, -0.22, 0.18)
    return jnp.clip(spiked(entries, jax.random.fold_in(rng, 3), *heavy), -limit, limit).astype(kind)


def setup_inputs(seed: int = 0) -> dict:
    key_list = jax.random.split(jax.random.key(seed), 10)
    return {
        "x_next": centred(key_list[0], (TOKENS, D), 1.0, 6.0, ((0, 32),)),
        "x_prev": centred(key_list[1], (TOKENS, D), 1.0, 6.0, ((0, 32),)),
        "grad_out": heavy_noise(key_list[2], (TOKENS, D), 1.0, 6.0, ((0, 32),), (0, 1, 32, 2.75)),
        "gate_w": centred(key_list[3], (D, FF), D ** -0.5, 0.125, ((0, 8), (1, 4))),
        "up_w": centred(key_list[4], (D, FF), D ** -0.5, 0.125, ((0, 8), (1, 4))),
        "down_w": centred(key_list[5], (FF, D), FF ** -0.5, 0.109375, ((0, 4), (1, 8))),
        "acc_gate": centred(key_list[6], (D, FF), 0.3, 2.5, ((0, 8), (1, 4)), jnp.float32),
        "acc_up": centred(key_list[7], (D, FF), 0.3, 2.5, ((0, 8), (1, 4)), jnp.float32),
        "acc_down": centred(key_list[8], (FF, D), 0.3, 2.5, ((0, 4), (1, 8)), jnp.float32),
    }


def block_sum(make_part):
    block = FF // N_TP
    total = None
    for index in range(N_TP):
        part = make_part(index * block, block)
        rounded = lax.optimization_barrier(part.astype(jnp.bfloat16)).astype(jnp.float32)
        total = rounded if total is None else total + rounded
    return total

def reference(x_next, x_prev, grad_out, gate_w, up_w, down_w, acc_gate, acc_up, acc_down):
    gate_next = jnp.dot(x_next, gate_w, preferred_element_type=jnp.float32)
    up_next = jnp.dot(x_next, up_w, preferred_element_type=jnp.float32)
    saved_hidden = (jax.nn.silu(gate_next) * up_next).astype(jnp.bfloat16)

    def out_part(start, width):
        return jnp.dot(saved_hidden[:, start:start + width], down_w[start:start + width], preferred_element_type=jnp.float32)
    out_next = block_sum(out_part).astype(jnp.bfloat16)
    gate_prev = jnp.dot(x_prev, gate_w, preferred_element_type=jnp.float32)
    up_prev = jnp.dot(x_prev, up_w, preferred_element_type=jnp.float32)
    grad_hidden = jnp.dot(grad_out, down_w.T, preferred_element_type=jnp.float32)
    sigmoid_gate = jax.nn.sigmoid(gate_prev)
    silu_gate = gate_prev * sigmoid_gate
    grad_gate = (grad_hidden * up_prev * sigmoid_gate * (1.0 + gate_prev * (1.0 - sigmoid_gate))).astype(jnp.bfloat16)
    grad_up = (grad_hidden * silu_gate).astype(jnp.bfloat16)
    hidden_prev = (silu_gate * up_prev).astype(jnp.bfloat16)

    def input_part(start, width):
        first = jnp.dot(grad_gate[:, start:start + width], gate_w[:, start:start + width].T, preferred_element_type=jnp.float32)
        second = jnp.dot(grad_up[:, start:start + width], up_w[:, start:start + width].T, preferred_element_type=jnp.float32)
        return first + second
    grad_input = block_sum(input_part).astype(jnp.bfloat16)
    factor = 1.0 / math.sqrt(TOKENS)
    new_gate = acc_gate + factor * jnp.dot(x_prev.T, grad_gate, preferred_element_type=jnp.float32)
    new_up = acc_up + factor * jnp.dot(x_prev.T, grad_up, preferred_element_type=jnp.float32)
    new_down = acc_down + factor * jnp.dot(hidden_prev.T, grad_out, preferred_element_type=jnp.float32)
    return (out_next, saved_hidden, grad_input, new_gate, new_up, new_down)
```

```python
import math

import jax
import jax.numpy as jnp
from jax import lax
from jax.experimental import pallas as pl
from jax.experimental.pallas import tpu as pltpu
from jax.sharding import PartitionSpec as P

MESH = pl.DeviceIdType.MESH
ANY = pl.BlockSpec(memory_space=pl.ANY)


def columns_of(size):
    side = 1
    while 8 * side * side <= size and size % (2 * side) == 0:
        side *= 2
    return side


def contract_rows(left, right):
    return lax.dot_general(
        left, right, (((0,), (0,)), ((), ())), preferred_element_type=jnp.float32
    )


def contract_cols(left, right):
    return lax.dot_general(
        left, right, (((1,), (1,)), ((), ())), preferred_element_type=jnp.float32
    )


def remote(source, target, send, recv, device):
    return pltpu.make_async_remote_copy(
        src_ref=source, dst_ref=target, send_sem=send, recv_sem=recv,
        device_id=device, device_id_type=MESH,
    )


class Spread:
    def __init__(self, fs, owns, fulls, send, recv):
        self.ny = columns_of(fs)
        self.nz = fs // self.ny
        self.fs, self.owns, self.fulls = fs, owns, fulls
        self.send, self.recv = send, recv
        self.f, self.t = lax.axis_index("fs"), lax.axis_index("tp")
        self.z, self.y = self.f // self.ny, lax.rem(self.f, self.ny)

    def flows(self, w, f, source, up, down, act):
        full = self.fulls[w].at[f]

        def go(kind, z, y):
            act(remote(source, full, self.send.at[w, kind, f], self.recv.at[w, f],
                       (z * self.ny + y, self.t)))

        if up:
            pl.when(self.z + 1 < self.nz)(lambda: go(0, self.z + 1, self.y))
        if down:
            pl.when(self.z > 0)(lambda: go(1, self.z - 1, self.y))
        for k in range(1, self.ny):
            go(1 + k, self.z, lax.rem(self.y + k, self.ny))

    def start(self):
        for w, own in enumerate(self.owns):
            self.flows(w, self.f, own, True, True, lambda c: c.start())

    def arrived(self, w, f):
        full = self.fulls[w].at[f]
        remote(full, full, self.send.at[w, 0, f], self.recv.at[w, f],
               (self.f, self.t)).wait_recv()

    def relay(self, act, wait):
        for d in range(1, self.nz):
            for w in range(len(self.owns)):
                def from_below(w=w, d=d):
                    f = (self.z - d) * self.ny + self.y
                    if wait:
                        self.arrived(w, f)
                    self.flows(w, f, self.fulls[w].at[f], True, False, act)

                def from_above(w=w, d=d):
                    f = (self.z + d) * self.ny + self.y
                    if wait:
                        self.arrived(w, f)
                    self.flows(w, f, self.fulls[w].at[f], False, True, act)

                pl.when(self.z >= d)(from_below)
                pl.when(self.z + d < self.nz)(from_above)

    def finish(self):
        for w in range(len(self.owns)):
            for z in range(self.nz):
                for k in range(1, self.ny):
                    self.arrived(w, z * self.ny + lax.rem(self.y + k, self.ny))
        for w, own in enumerate(self.owns):
            self.flows(w, self.f, own, True, True, lambda c: c.wait_send())
        self.relay(lambda c: c.wait_send(), False)


def stage_in(pairs, sem):
    copies = [pltpu.make_async_copy(a, b, sem.at[i]) for i, (a, b) in enumerate(pairs)]
    for copy in copies:
        copy.start()
    return copies


def gather_inputs(fs, tp, *refs):
    (gate, up, down, xn, xp, go, cols,
     gate_o, up_o, down_o, xn_o, xp_o, go_o, cols_o,
     *rest) = refs
    held, (wsend, wrecv, tsend, trecv, csend, crecv, dsend, drecv, lin, lout) = rest[:7], rest[7:]
    f, t = lax.axis_index("fs"), lax.axis_index("tp")
    sources = (gate, up, down, xn, xp, go, cols)
    into = stage_in(list(zip(sources, held)), lin)
    spread = Spread(fs, held[:3], (gate_o, up_o, down_o), wsend, wrecv)
    for copy in into[:3]:
        copy.wait()
    spread.start()
    for copy in into[3:]:
        copy.wait()
    tokens = ((held[3], xn_o), (held[4], xp_o), (held[5], go_o))
    token_copies = [
        remote(a, b.at[t], tsend.at[i, k], trecv.at[i, t], (f, lax.rem(t + k, tp)))
        for i, (a, b) in enumerate(tokens) for k in range(1, tp)
    ]
    slices = held[6]
    slice_copies = []
    for k in range(1, fs):
        other = lax.rem(f + k, fs)
        slice_copies.append(
            remote(slices.at[other], cols_o.at[f, t], csend.at[k], crecv.at[f], (other, t)))
    for copy in token_copies + slice_copies:
        copy.start()
    out = stage_in(
        [(held[0], gate_o.at[f]), (held[1], up_o.at[f]), (held[2], down_o.at[f]),
         (held[3], xn_o.at[t]), (held[4], xp_o.at[t]), (held[5], go_o.at[t]),
         (slices.at[f], cols_o.at[f, t])], lout)
    spread.relay(lambda c: c.start(), True)
    out[6].wait()
    for k in range(1, fs):
        other = lax.rem(f + k, fs)
        mine = cols_o.at[other, t]
        remote(mine, mine, csend.at[k], crecv.at[other], (f, t)).wait_recv()
    mine = cols_o.at[:, t]
    share = [remote(mine, mine, dsend.at[k], drecv.at[t], (f, lax.rem(t + k, tp)))
             for k in range(1, tp)]
    for copy in share:
        copy.start()
    for k in range(1, tp):
        other = lax.rem(t + k, tp)
        for i, (_, b) in enumerate(tokens):
            remote(b.at[other], b.at[other], tsend.at[i, k], trecv.at[i, other], (f, t)).wait_recv()
        theirs = cols_o.at[:, other]
        remote(theirs, theirs, dsend.at[k], drecv.at[other], (f, t)).wait_recv()
    spread.finish()
    for copy in token_copies + slice_copies + share:
        copy.wait_send()
    for copy in out[:6]:
        copy.wait()


def gather_terms(fs, tp, *refs):
    (gg, gu, hp, pn, pp, gg_o, gu_o, hp_o, pn_o, pp_o, *rest) = refs
    held, (wsend, wrecv, tsend, trecv, lin, lout) = rest[:5], rest[5:]
    f, t = lax.axis_index("fs"), lax.axis_index("tp")
    into = stage_in(list(zip((gg, gu, hp, pn, pp), held)), lin)
    spread = Spread(fs, held[:3], (gg_o, gu_o, hp_o), wsend, wrecv)
    for copy in into[:3]:
        copy.wait()
    spread.start()
    for copy in into[3:]:
        copy.wait()
    parts = ((held[3], pn_o), (held[4], pp_o))
    part_copies = []
    for i, (a, b) in enumerate(parts):
        for k in range(1, tp):
            other = lax.rem(t + k, tp)
            part_copies.append(
                remote(a.at[other], b.at[t], tsend.at[i, k], trecv.at[i, t], (f, other)))
    for copy in part_copies:
        copy.start()
    out = stage_in(
        [(held[0], gg_o.at[f]), (held[1], gu_o.at[f]), (held[2], hp_o.at[f]),
         (held[3].at[t], pn_o.at[t]), (held[4].at[t], pp_o.at[t])], lout)
    spread.relay(lambda c: c.start(), True)
    for i, (_, b) in enumerate(parts):
        for k in range(1, tp):
            other = lax.rem(t + k, tp)
            remote(b.at[other], b.at[other], tsend.at[i, k], trecv.at[i, other], (f, t)).wait_recv()
    spread.finish()
    for copy in part_copies:
        copy.wait_send()
    for copy in out:
        copy.wait()


def communicate(body, fs, tp, args, shapes, extra, name):
    n = len(args)
    return pl.pallas_call(
        lambda *refs: body(fs, tp, *refs),
        out_shape=[jax.ShapeDtypeStruct(s, jnp.bfloat16) for s in shapes],
        in_specs=[ANY] * n,
        out_specs=[ANY] * len(shapes),
        scratch_shapes=[pltpu.VMEM(a.shape, a.dtype) for a in args]
        + [pltpu.SemaphoreType.DMA((3, columns_of(fs) + 1, fs)), pltpu.SemaphoreType.DMA((3, fs)),
           pltpu.SemaphoreType.DMA((3, tp)), pltpu.SemaphoreType.DMA((3, tp))]
        + extra
        + [pltpu.SemaphoreType.DMA((n,)), pltpu.SemaphoreType.DMA((n,))],
        compiler_params=pltpu.CompilerParams(has_side_effects=True),
        name=name,
    )(*args)


def local(x_next, x_prev, grad_out, gate_w, up_w, down_w, acc_gate, acc_up, acc_down):
    fs, tp = lax.axis_size("fs"), lax.axis_size("tp")
    rows, model = x_prev.shape
    depth, width = gate_w.shape
    factor = 1.0 / math.sqrt(rows * tp * fs)
    cols = jnp.concatenate(
        (x_prev.reshape(rows, fs, depth), grad_out.reshape(rows, fs, depth)), axis=2
    ).transpose(1, 0, 2)
    sems = pltpu.SemaphoreType.DMA
    gate_full, up_full, down_full, piece, rows_prev, cotangent, all_cols = communicate(
        gather_inputs, fs, tp, (gate_w, up_w, down_w, x_next, x_prev, grad_out, cols),
        [(fs, depth, width), (fs, depth, width), (fs, width, depth)]
        + [(tp, rows, model)] * 3 + [(fs, tp, rows, 2 * depth)],
        [sems((fs,)), sems((fs,)), sems((tp,)), sems((tp,))], "gather_inputs",
    )
    gate_full, up_full = gate_full.reshape(model, width), up_full.reshape(model, width)
    down_full = down_full.transpose(1, 0, 2).reshape(width, model)
    piece, rows_prev, cotangent = (a.reshape(tp * rows, model) for a in (piece, rows_prev, cotangent))
    x_cols = all_cols[..., :depth].reshape(fs * tp * rows, depth)
    g_cols = all_cols[..., depth:].reshape(fs * tp * rows, depth)

    gate = jnp.dot(piece, gate_full, preferred_element_type=jnp.float32)
    upper = jnp.dot(piece, up_full, preferred_element_type=jnp.float32)
    hidden = (jax.nn.silu(gate) * upper).astype(jnp.bfloat16)
    part_next = jnp.dot(hidden, down_full, preferred_element_type=jnp.float32).astype(jnp.bfloat16)
    gate_prev = jnp.dot(rows_prev, gate_full, preferred_element_type=jnp.float32)
    up_prev = jnp.dot(rows_prev, up_full, preferred_element_type=jnp.float32)
    grad_hidden = contract_cols(cotangent, down_full)
    sigmoid_gate = jax.nn.sigmoid(gate_prev)
    silu_gate = gate_prev * sigmoid_gate
    grad_gate = (
        grad_hidden * up_prev * sigmoid_gate * (1.0 + gate_prev * (1.0 - sigmoid_gate))
    ).astype(jnp.bfloat16)
    grad_up = (grad_hidden * silu_gate).astype(jnp.bfloat16)
    hidden_prev = (silu_gate * up_prev).astype(jnp.bfloat16)
    part_prev = (contract_cols(grad_gate, gate_full) + contract_cols(grad_up, up_full)).astype(jnp.bfloat16)

    all_gate, all_up, all_hidden, parts_next, parts_prev = communicate(
        gather_terms, fs, tp,
        (grad_gate, grad_up, hidden_prev,
         part_next.reshape(tp, rows, model), part_prev.reshape(tp, rows, model)),
        [(fs, tp * rows, width)] * 3 + [(tp, rows, model)] * 2, [], "gather_terms",
    )
    all_gate, all_up, all_hidden = (a.reshape(fs * tp * rows, width) for a in (all_gate, all_up, all_hidden))
    new_gate = acc_gate + factor * contract_rows(x_cols, all_gate)
    new_up = acc_up + factor * contract_rows(x_cols, all_up)
    new_down = acc_down + factor * contract_rows(all_hidden, g_cols)
    summed = parts_next.astype(jnp.float32).sum(0).astype(jnp.bfloat16)
    grad_input = parts_prev.astype(jnp.float32).sum(0).astype(jnp.bfloat16)
    return (summed, hidden, grad_input, new_gate, new_up, new_down)


def solution(mesh):
    in_specs = (
        P(("fs", "tp"), None),
        P(("fs", "tp"), None),
        P(("fs", "tp"), None),
        P("fs", "tp"),
        P("fs", "tp"),
        P("tp", "fs"),
        P("fs", "tp"),
        P("fs", "tp"),
        P("tp", "fs"),
    )
    out_specs = (
        P(("fs", "tp"), None),
        P("fs", "tp"),
        P(("fs", "tp"), None),
        P("fs", "tp"),
        P("fs", "tp"),
        P("tp", "fs"),
    )
    return jax.shard_map(local, mesh=mesh, in_specs=in_specs, out_specs=out_specs, check_vma=False)
```

```python
import math

import jax
import jax.numpy as jnp
from jax import lax
from jax.experimental import pallas as pl
from jax.experimental.pallas import tpu as pltpu
from jax.sharding import PartitionSpec as P

MESH = pl.DeviceIdType.MESH
ANY = pl.BlockSpec(memory_space=pl.ANY)


def columns_of(size):
    side = 1
    while 8 * side * side <= size and size % (2 * side) == 0:
        side *= 2
    return side


def contract_rows(left, right):
    return lax.dot_general(
        left, right, (((0,), (0,)), ((), ())), preferred_element_type=jnp.float32
    )


def contract_cols(left, right):
    return lax.dot_general(
        left, right, (((1,), (1,)), ((), ())), preferred_element_type=jnp.float32
    )


def remote(source, target, send, recv, device):
    return pltpu.make_async_remote_copy(
        src_ref=source, dst_ref=target, send_sem=send, recv_sem=recv,
        device_id=device, device_id_type=MESH,
    )


class Spread:
    def __init__(self, fs, owns, fulls, send, recv):
        self.ny = columns_of(fs)
        self.nz = fs // self.ny
        self.fs, self.owns, self.fulls = fs, owns, fulls
        self.send, self.recv = send, recv
        self.f, self.t = lax.axis_index("fs"), lax.axis_index("tp")
        self.z, self.y = self.f // self.ny, lax.rem(self.f, self.ny)

    def flows(self, w, f, source, up, down, act):
        full = self.fulls[w].at[f]

        def go(kind, z, y):
            act(remote(source, full, self.send.at[w, kind, f], self.recv.at[w, f],
                       (z * self.ny + y, self.t)))

        if up:
            pl.when(self.z + 1 < self.nz)(lambda: go(0, self.z + 1, self.y))
        if down:
            pl.when(self.z > 0)(lambda: go(1, self.z - 1, self.y))
        for k in range(1, self.ny):
            go(1 + k, self.z, lax.rem(self.y + k, self.ny))

    def start(self):
        for w, own in enumerate(self.owns):
            self.flows(w, self.f, own, True, True, lambda c: c.start())

    def arrived(self, w, f):
        full = self.fulls[w].at[f]
        remote(full, full, self.send.at[w, 0, f], self.recv.at[w, f],
               (self.f, self.t)).wait_recv()

    def relay(self, act, wait):
        for d in range(1, self.nz):
            for w in range(len(self.owns)):
                def from_below(w=w, d=d):
                    f = (self.z - d) * self.ny + self.y
                    if wait:
                        self.arrived(w, f)
                    self.flows(w, f, self.fulls[w].at[f], True, False, act)

                def from_above(w=w, d=d):
                    f = (self.z + d) * self.ny + self.y
                    if wait:
                        self.arrived(w, f)
                    self.flows(w, f, self.fulls[w].at[f], False, True, act)

                pl.when(self.z >= d)(from_below)
                pl.when(self.z + d < self.nz)(from_above)

    def finish(self):
        for w in range(len(self.owns)):
            for z in range(self.nz):
                for k in range(1, self.ny):
                    self.arrived(w, z * self.ny + lax.rem(self.y + k, self.ny))
        for w, own in enumerate(self.owns):
            self.flows(w, self.f, own, True, True, lambda c: c.wait_send())
        self.relay(lambda c: c.wait_send(), False)


def stage_in(pairs, sem):
    copies = [pltpu.make_async_copy(a, b, sem.at[i]) for i, (a, b) in enumerate(pairs)]
    for copy in copies:
        copy.start()
    return copies


def gather_inputs(fs, tp, *refs):
    (gate, up, down, xn, xp, go, cols,
     gate_o, up_o, down_o, xn_o, xp_o, go_o, cols_o,
     *rest) = refs
    held, (wsend, wrecv, tsend, trecv, csend, crecv, dsend, drecv, lin, lout) = rest[:7], rest[7:]
    f, t = lax.axis_index("fs"), lax.axis_index("tp")
    sources = (gate, up, down, xn, xp, go, cols)
    into = stage_in(list(zip(sources, held)), lin)
    spread = Spread(fs, held[:3], (gate_o, up_o, down_o), wsend, wrecv)
    for copy in into[:3]:
        copy.wait()
    spread.start()
    for copy in into[3:]:
        copy.wait()
    tokens = ((held[3], xn_o), (held[4], xp_o), (held[5], go_o))
    token_copies = [
        remote(a, b.at[t], tsend.at[i, k], trecv.at[i, t], (f, lax.rem(t + k, tp)))
        for i, (a, b) in enumerate(tokens) for k in range(1, tp)
    ]
    slices = held[6]
    slice_copies = []
    for k in range(1, fs):
        other = lax.rem(f + k, fs)
        slice_copies.append(
            remote(slices.at[other], cols_o.at[f, t], csend.at[k], crecv.at[f], (other, t)))
    for copy in token_copies + slice_copies:
        copy.start()
    out = stage_in(
        [(held[0], gate_o.at[f]), (held[1], up_o.at[f]), (held[2], down_o.at[f]),
         (held[3], xn_o.at[t]), (held[4], xp_o.at[t]), (held[5], go_o.at[t]),
         (slices.at[f], cols_o.at[f, t])], lout)
    spread.relay(lambda c: c.start(), True)
    out[6].wait()
    for k in range(1, fs):
        other = lax.rem(f + k, fs)
        mine = cols_o.at[other, t]
        remote(mine, mine, csend.at[k], crecv.at[other], (f, t)).wait_recv()
    mine = cols_o.at[:, t]
    share = [remote(mine, mine, dsend.at[k], drecv.at[t], (f, lax.rem(t + k, tp)))
             for k in range(1, tp)]
    for copy in share:
        copy.start()
    for k in range(1, tp):
        other = lax.rem(t + k, tp)
        for i, (_, b) in enumerate(tokens):
            remote(b.at[other], b.at[other], tsend.at[i, k], trecv.at[i, other], (f, t)).wait_recv()
        theirs = cols_o.at[:, other]
        remote(theirs, theirs, dsend.at[k], drecv.at[other], (f, t)).wait_recv()
    spread.finish()
    for copy in token_copies + slice_copies + share:
        copy.wait_send()
    for copy in out[:6]:
        copy.wait()


def gather_terms(fs, tp, *refs):
    (gg, gu, hp, pn, pp, gg_o, gu_o, hp_o, pn_o, pp_o, *rest) = refs
    held, (wsend, wrecv, tsend, trecv, lin, lout) = rest[:5], rest[5:]
    f, t = lax.axis_index("fs"), lax.axis_index("tp")
    into = stage_in(list(zip((gg, gu, hp, pn, pp), held)), lin)
    spread = Spread(fs, held[:3], (gg_o, gu_o, hp_o), wsend, wrecv)
    for copy in into[:3]:
        copy.wait()
    spread.start()
    for copy in into[3:]:
        copy.wait()
    parts = ((held[3], pn_o), (held[4], pp_o))
    part_copies = []
    for i, (a, b) in enumerate(parts):
        for k in range(1, tp):
            other = lax.rem(t + k, tp)
            part_copies.append(
                remote(a.at[other], b.at[t], tsend.at[i, k], trecv.at[i, t], (f, other)))
    for copy in part_copies:
        copy.start()
    out = stage_in(
        [(held[0], gg_o.at[f]), (held[1], gu_o.at[f]), (held[2], hp_o.at[f]),
         (held[3].at[t], pn_o.at[t]), (held[4].at[t], pp_o.at[t])], lout)
    spread.relay(lambda c: c.start(), True)
    for i, (_, b) in enumerate(parts):
        for k in range(1, tp):
            other = lax.rem(t + k, tp)
            remote(b.at[other], b.at[other], tsend.at[i, k], trecv.at[i, other], (f, t)).wait_recv()
    spread.finish()
    for copy in part_copies:
        copy.wait_send()
    for copy in out:
        copy.wait()


def communicate(body, fs, tp, args, shapes, extra, name):
    n = len(args)
    return pl.pallas_call(
        lambda *refs: body(fs, tp, *refs),
        out_shape=[jax.ShapeDtypeStruct(s, jnp.bfloat16) for s in shapes],
        in_specs=[ANY] * n,
        out_specs=[ANY] * len(shapes),
        scratch_shapes=[pltpu.VMEM(a.shape, a.dtype) for a in args]
        + [pltpu.SemaphoreType.DMA((3, columns_of(fs) + 1, fs)), pltpu.SemaphoreType.DMA((3, fs)),
           pltpu.SemaphoreType.DMA((3, tp)), pltpu.SemaphoreType.DMA((3, tp))]
        + extra
        + [pltpu.SemaphoreType.DMA((n,)), pltpu.SemaphoreType.DMA((n,))],
        compiler_params=pltpu.CompilerParams(has_side_effects=True),
        name=name,
    )(*args)


def local(x_next, x_prev, grad_out, gate_w, up_w, down_w, acc_gate, acc_up, acc_down):
    fs, tp = lax.axis_size("fs"), lax.axis_size("tp")
    rows, model = x_prev.shape
    depth, width = gate_w.shape
    factor = 1.0 / math.sqrt(rows * tp * fs)
    cols = jnp.concatenate(
        (x_prev.reshape(rows, fs, depth), grad_out.reshape(rows, fs, depth)), axis=2
    ).transpose(1, 0, 2)
    sems = pltpu.SemaphoreType.DMA
    gate_full, up_full, down_full, piece, rows_prev, cotangent, all_cols = communicate(
        gather_inputs, fs, tp, (gate_w.T, up_w.T, down_w, x_next, x_prev, grad_out, cols),
        [(fs, width, depth)] * 3
        + [(tp, rows, model)] * 3 + [(fs, tp, rows, 2 * depth)],
        [sems((fs,)), sems((fs,)), sems((tp,)), sems((tp,))], "gather_inputs",
    )
    gate_full, up_full, down_full = (
        a.transpose(1, 0, 2).reshape(width, model) for a in (gate_full, up_full, down_full)
    )
    piece, rows_prev, cotangent = (a.reshape(tp * rows, model) for a in (piece, rows_prev, cotangent))
    x_cols = all_cols[..., :depth].reshape(fs * tp * rows, depth)
    g_cols = all_cols[..., depth:].reshape(fs * tp * rows, depth)

    gate, upper = contract_cols(piece, gate_full), contract_cols(piece, up_full)
    hidden = (jax.nn.silu(gate) * upper).astype(jnp.bfloat16)
    part_next = jnp.dot(hidden, down_full, preferred_element_type=jnp.float32).astype(jnp.bfloat16)
    gate_prev, up_prev = contract_cols(rows_prev, gate_full), contract_cols(rows_prev, up_full)
    grad_hidden = contract_cols(cotangent, down_full)
    sigmoid_gate = jax.nn.sigmoid(gate_prev)
    silu_gate = gate_prev * sigmoid_gate
    grad_gate = (
        grad_hidden * up_prev * sigmoid_gate * (1.0 + gate_prev * (1.0 - sigmoid_gate))
    ).astype(jnp.bfloat16)
    grad_up = (grad_hidden * silu_gate).astype(jnp.bfloat16)
    hidden_prev = (silu_gate * up_prev).astype(jnp.bfloat16)
    part_prev = (
        jnp.dot(grad_gate, gate_full, preferred_element_type=jnp.float32)
        + jnp.dot(grad_up, up_full, preferred_element_type=jnp.float32)
    ).astype(jnp.bfloat16)

    all_gate, all_up, all_hidden, parts_next, parts_prev = communicate(
        gather_terms, fs, tp,
        (grad_gate, grad_up, hidden_prev,
         part_next.reshape(tp, rows, model), part_prev.reshape(tp, rows, model)),
        [(fs, tp * rows, width)] * 3 + [(tp, rows, model)] * 2, [], "gather_terms",
    )
    all_gate, all_up, all_hidden = (a.reshape(fs * tp * rows, width) for a in (all_gate, all_up, all_hidden))
    new_gate = acc_gate + factor * contract_rows(x_cols, all_gate)
    new_up = acc_up + factor * contract_rows(x_cols, all_up)
    new_down = acc_down + factor * contract_rows(all_hidden, g_cols)
    summed = parts_next.astype(jnp.float32).sum(0).astype(jnp.bfloat16)
    grad_input = parts_prev.astype(jnp.float32).sum(0).astype(jnp.bfloat16)
    return (summed, hidden, grad_input, new_gate, new_up, new_down)


def solution(mesh):
    in_specs = (
        P(("fs", "tp"), None),
        P(("fs", "tp"), None),
        P(("fs", "tp"), None),
        P("fs", "tp"),
        P("fs", "tp"),
        P("tp", "fs"),
        P("fs", "tp"),
        P("fs", "tp"),
        P("tp", "fs"),
    )
    out_specs = (
        P(("fs", "tp"), None),
        P("fs", "tp"),
        P(("fs", "tp"), None),
        P("fs", "tp"),
        P("fs", "tp"),
        P("tp", "fs"),
    )
    return jax.shard_map(local, mesh=mesh, in_specs=in_specs, out_specs=out_specs, check_vma=False)
```
